32 devices in a mesh: sp: 8 (over z, y), tp: 4 (over x, core).
Axes of the slice: x: 2, y: 2, z: 4, core: 2. Of those that a mesh axis runs over, the one named last changes fastest.
Arguments:
- query_rows: bfloat16 [4096, 1024], P('sp', 'tp'), may hold values from -6 to 6
- key_rows: bfloat16 [4096, 512], P('sp', 'tp'), may hold values from -6 to 6
- value_rows: bfloat16 [4096, 512], P('sp', 'tp'), may hold values from -12 to 12
- query_gain: float32 [128], replicated, may hold values from 0.2 to 6.5
- key_gain: float32 [128], replicated, may hold values from 0.2 to 6.5
- residual: bfloat16 [4096, 2048], P(('sp', 'tp')), may hold values from -6 to 6
- out_weight: bfloat16 [1024, 2048], P('tp'), may hold values from -3 to 3
- mix_gain: float32 [2048], replicated, may hold values from 0.1 to 1.9
- gate_weight: bfloat16 [2048, 5632], P('sp', 'tp'), may hold values from -0.125 to 0.125
- up_weight: bfloat16 [2048, 5632], P('sp', 'tp'), may hold values from -0.125 to 0.125
- down_weight: bfloat16 [5632, 2048], P('tp', 'sp'), may hold values from -0.15625 to 0.15625
Outputs:
- layer_out: bfloat16 [4096, 2048], P(('sp', 'tp'))
The draws below stay inside these ranges and needn't reach their ends.
All inputs are finite; a program needn't handle non-finite values.
Results may differ from the reference program's by a relative error of at most 0.015.
The reference program's roundings to bfloat16 on the way count: a program that leaves them out, or rounds other values in their place, can miss the bound.
Values may be sent and summed in bfloat16 or wider, within the bound.
A program may use at most 128 MiB of HBM per device.

```python
import jax
import jax.numpy as jnp
from jax import lax

D = 2048
HD = 128
QHEADS = 8
KVHEADS = 4
FF = 5632
GRID = 64
TOK_DEV = 512
TOKENS = 4096
N_TP = 4


def drawn_keys(key):
    base_keys = jnp.clip(jax.random.normal(jax.random.fold_in(key, 11), (TOKENS, KVHEADS * HD), jnp.float32), -6.0, 6.0)
    return base_keys


def draw_key_rows(key, part):
    return drawn_keys(key).astype(jnp.bfloat16)


def draw_query_rows(key, part):
    fresh = jnp.clip(jax.random.normal(jax.random.fold_in(key, 23), (TOKENS, QHEADS * HD), jnp.float32), -6.0, 6.0)
    return fresh.astype(jnp.bfloat16)


def gain_values(key):
    return 1.0 + 0.18 * jnp.clip(jax.random.normal(key, (HD,), jnp.float32), -4.4, 4.4)


def draw_query_gain(key, part):
    return gain_values(jax.random.fold_in(key, 31))


def draw_key_gain(key, part):
    return gain_values(jax.random.fold_in(key, 37))


def draw_out_weight(key, part):
    fresh = jnp.clip(jax.random.normal(jax.random.fold_in(key, 41), (QHEADS * HD, D), jnp.float32), -6.0, 6.0)
    spread = 0.5
    return (fresh * spread).astype(jnp.bfloat16)


def level_of(own_key, extent, pieces, least, largest):
    factor_of, own = 1.0, jax.random.fold_in(own_key, 6)
    for dim, shards_of in pieces:
        heights = jnp.exp(jax.random.uniform(jax.random.fold_in(own, dim), (shards_of,), jnp.float32, least / len(pieces), largest / len(pieces)))
        factor_of = factor_of * jnp.repeat(heights, extent[dim] // shards_of).reshape([-1 if axis == dim else 1 for axis in range(len(extent))])
    return factor_of


def bell_draw(own_key, dims, deviation, limit, cuts=(), kind=jnp.bfloat16):
    result = deviation * jax.random.normal(own_key, dims, jnp.float32)
    if cuts:
        result = result * level_of(own_key, dims, cuts, -0.22, 0.18)
    return jnp.clip(result, -limit, limit).astype(kind)


def setup_inputs(seed: int = 0) -> dict:
    keys = jax.random.split(jax.random.key(seed), 12)
    return {
        "query_rows": draw_query_rows(jax.random.fold_in(keys[11], 71), 0),
        "key_rows": draw_key_rows(jax.random.fold_in(keys[11], 71), 0),
        "value_rows": bell_draw(keys[2], (TOKENS, KVHEADS * HD), 2.0, 12.0, ((0, 8), (1, 4))),
        "query_gain": draw_query_gain(jax.random.fold_in(keys[11], 71), 0),
        "key_gain": draw_key_gain(jax.random.fold_in(keys[11], 71), 0),
        "residual": bell_draw(keys[5], (TOKENS, D), 1.0, 6.0, ((0, 32),)),
        "out_weight": draw_out_weight(jax.random.fold_in(keys[11], 71), 0),
        "mix_gain": jnp.clip(1.0 + 0.18 * jax.random.normal(keys[7], (D,), jnp.float32), 0.1, 1.9),
        "gate_weight": bell_draw(keys[8], (D, FF), D ** -0.5, 0.125, ((0, 8), (1, 4))),
        "up_weight": bell_draw(keys[9], (D, FF), D ** -0.5, 0.125, ((0, 8), (1, 4))),
        "down_weight": bell_draw(keys[10], (FF, D), (FF // 4) ** -0.5, 0.15625, ((0, 4), (1, 8))),
    }


norm_eps = 1e-06
theta_base = 10000.0

def spin(halfway, angles):
    cosine = jnp.cos(angles)[:, None, :]
    sine_val = jnp.sin(angles)[:, None, :]
    quarter = halfway.shape[-1] // 2
    leading = halfway[..., :quarter]
    trailing = halfway[..., quarter:]
    return [leading * cosine - trailing * sine_val, trailing * cosine + leading * sine_val]

def rotate_grid(vectors, positions):
    head_dim = vectors.shape[-1]
    quarter = head_dim // 4
    frequency = jnp.power(theta_base, -2.0 * jnp.arange(quarter, dtype=jnp.float32) / (head_dim // 2))
    row_angle = (positions // GRID).astype(jnp.float32)[:, None] * frequency
    col_angle = (positions % GRID).astype(jnp.float32)[:, None] * frequency
    lower_half = vectors[..., :2 * quarter]
    upper_half = vectors[..., 2 * quarter:]
    return jnp.concatenate(spin(lower_half, row_angle) + spin(upper_half, col_angle), axis=-1)

def prepare_heads(raw_heads, head_gain, positions):
    floated = raw_heads.astype(jnp.float32)
    scaled = floated * lax.rsqrt(lax.optimization_barrier(jnp.mean(floated * floated, axis=-1, keepdims=True)) + norm_eps)
    return rotate_grid(scaled * head_gain, positions).astype(jnp.bfloat16)

def row_norm(row_data, row_gain):
    floated = row_data.astype(jnp.float32)
    scaled = floated * lax.rsqrt(lax.optimization_barrier(jnp.mean(floated * floated, axis=-1, keepdims=True)) + norm_eps)
    return (scaled * row_gain).astype(jnp.bfloat16)

def to_wire(partial_value):
    return lax.optimization_barrier(partial_value.astype(jnp.bfloat16)).astype(jnp.float32)

def reference(query_rows, key_rows, value_rows, query_gain, key_gain, residual, out_weight, mix_gain, gate_weight, up_weight, down_weight):
    positions = jnp.arange(TOKENS, dtype=jnp.int32)
    group_size = QHEADS // KVHEADS
    q_heads = prepare_heads(query_rows.reshape(TOKENS, QHEADS, HD), query_gain, positions)
    k_heads = prepare_heads(key_rows.reshape(TOKENS, KVHEADS, HD), key_gain, positions).astype(jnp.float32)
    v_heads = value_rows.reshape(TOKENS, KVHEADS, HD).astype(jnp.float32)
    score_scale = HD ** (-0.5)
    q_blocks = q_heads.reshape(TOKENS // TOK_DEV, TOK_DEV, KVHEADS, group_size, HD)

    def attend(query_block):
        scores = jnp.einsum('qkgd,skd->kgqs', query_block.astype(jnp.float32), k_heads) * score_scale
        row_max = lax.optimization_barrier(jnp.max(scores, axis=-1, keepdims=True))
        weights = jnp.exp(scores - row_max)
        row_sum = lax.optimization_barrier(jnp.sum(weights, axis=-1))
        narrow = lax.optimization_barrier(weights.astype(jnp.bfloat16)).astype(jnp.float32)
        combined = jnp.einsum('kgqs,skd->qkgd', narrow, v_heads)
        return (combined / jnp.transpose(row_sum, (2, 0, 1))[..., None]).astype(jnp.bfloat16)
    attended = lax.map(attend, q_blocks).reshape(TOKENS, QHEADS * HD)
    head_cols = QHEADS * HD // N_TP
    attn_sum = jnp.zeros((TOKENS, D), jnp.float32)
    for member in range(N_TP):
        partial_value = jnp.dot(attended[:, member * head_cols:(member + 1) * head_cols], out_weight[member * head_cols:(member + 1) * head_cols], preferred_element_type=jnp.float32)
        attn_sum = attn_sum + to_wire(partial_value)
    updated = (residual.astype(jnp.float32) + attn_sum).astype(jnp.bfloat16)
    normed = row_norm(updated, mix_gain)
    unit_cols = FF // N_TP
    unit_sum = jnp.zeros((TOKENS, D), jnp.float32)
    for member in range(N_TP):
        gate_act = jnp.dot(normed, gate_weight[:, member * unit_cols:(member + 1) * unit_cols], preferred_element_type=jnp.float32)
        up_act = jnp.dot(normed, up_weight[:, member * unit_cols:(member + 1) * unit_cols], preferred_element_type=jnp.float32)
        hidden = (jax.nn.silu(gate_act) * up_act).astype(jnp.bfloat16)
        partial_value = jnp.dot(hidden, down_weight[member * unit_cols:(member + 1) * unit_cols], preferred_element_type=jnp.float32)
        unit_sum = unit_sum + to_wire(partial_value)
    return (updated.astype(jnp.float32) + 0.5 * unit_sum).astype(jnp.bfloat16)
```

```python
import functools
import math

import jax
import jax.numpy as jnp
from jax import lax
from jax.experimental import pallas as pl
from jax.experimental.pallas import tpu as pltpu
from jax.sharding import PartitionSpec as P

GRID = 64

norm_eps = 1e-06
theta_base = 10000.0


def spin(halfway, angles):
    cosine = jnp.cos(angles)[:, None, :]
    sine_val = jnp.sin(angles)[:, None, :]
    quarter = halfway.shape[-1] // 2
    leading = halfway[..., :quarter]
    trailing = halfway[..., quarter:]
    return [leading * cosine - trailing * sine_val, trailing * cosine + leading * sine_val]


def rotate_grid(vectors, positions):
    head_dim = vectors.shape[-1]
    quarter = head_dim // 4
    frequency = jnp.power(
        theta_base, -2.0 * jnp.arange(quarter, dtype=jnp.float32) / (head_dim // 2)
    )
    row_angle = (positions // GRID).astype(jnp.float32)[:, None] * frequency
    col_angle = (positions % GRID).astype(jnp.float32)[:, None] * frequency
    lower_half = vectors[..., : 2 * quarter]
    upper_half = vectors[..., 2 * quarter :]
    return jnp.concatenate(spin(lower_half, row_angle) + spin(upper_half, col_angle), axis=-1)


def prepare_heads(raw_heads, head_gain, positions):
    floated = raw_heads.astype(jnp.float32)
    scaled = floated * lax.rsqrt(jnp.mean(floated * floated, axis=-1, keepdims=True) + norm_eps)
    return rotate_grid(scaled * head_gain, positions).astype(jnp.bfloat16)


def row_norm(row_data, row_gain):
    floated = row_data.astype(jnp.float32)
    scaled = floated * lax.rsqrt(jnp.mean(floated * floated, axis=-1, keepdims=True) + norm_eps)
    return (scaled * row_gain).astype(jnp.bfloat16)


def attend_body(factor, q_ref, k_ref, v_ref, o_ref):
    scores = lax.dot_general(
        q_ref[0], k_ref[0], (((1,), (1,)), ((), ())), preferred_element_type=jnp.float32
    )
    top = jnp.max(scores, axis=-1, keepdims=True)
    weights = jnp.exp2((scores - top) * factor)
    total = jnp.sum(weights, axis=-1, keepdims=True)
    mixed = jnp.dot(weights.astype(jnp.bfloat16), v_ref[0], preferred_element_type=jnp.float32)
    o_ref[0] = (mixed / total).astype(o_ref.dtype)


def attend(q_stack, keys, values):
    local_kv, rows, head_dim = q_stack.shape
    count = keys.shape[1]
    tile = min(256, rows)
    return pl.pallas_call(
        functools.partial(attend_body, head_dim**-0.5 * math.log2(math.e)),
        grid=(local_kv, rows // tile),
        in_specs=[
            pl.BlockSpec((1, tile, head_dim), lambda h, i: (h, i, 0)),
            pl.BlockSpec((1, count, head_dim), lambda h, i: (h, 0, 0)),
            pl.BlockSpec((1, count, head_dim), lambda h, i: (h, 0, 0)),
        ],
        out_specs=pl.BlockSpec((1, tile, head_dim), lambda h, i: (h, i, 0)),
        out_shape=jax.ShapeDtypeStruct((local_kv, rows, head_dim), jnp.bfloat16),
        compiler_params=pltpu.CompilerParams(vmem_limit_bytes=40 * 1024 * 1024),
        cost_estimate=pl.CostEstimate(
            flops=4 * local_kv * rows * count * head_dim,
            bytes_accessed=4 * local_kv * (rows + count) * head_dim,
            transcendentals=local_kv * rows * count,
        ),
    )(q_stack, keys, values)


def on_device(
    sp_size,
    tp_size,
    query_rows,
    key_rows,
    value_rows,
    query_gain,
    key_gain,
    residual,
    out_weight,
    mix_gain,
    gate_weight,
    up_weight,
    down_weight,
):
    ring = list(range(0, sp_size, 2)) + list(range(1, sp_size, 2))[::-1]
    onward = [(ring[i], ring[(i + 1) % sp_size]) for i in range(sp_size)]
    backward = [(b, a) for a, b in onward]
    where = [ring.index(i) for i in range(sp_size)]
    my_place = jnp.asarray(where, jnp.int32)[lax.axis_index("sp")]
    ring_index = jnp.asarray(ring, jnp.int32)

    def owner(k):
        return ring_index[lax.rem(my_place + (k + 2 * sp_size), sp_size)]

    def travel(piece, perm, steps):
        out = []
        for _ in range(steps):
            piece = lax.ppermute(piece, "sp", perm)
            out.append(piece)
        return out

    def partner(piece, d):
        return lax.ppermute(piece, "tp", [(t, t ^ d) for t in range(tp_size)])

    tok_rows = query_rows.shape[0]
    head_dim = query_gain.shape[0]
    local_kv = key_rows.shape[1] // head_dim
    local_q = query_rows.shape[1] // head_dim
    group_size = local_q // local_kv
    positions = lax.axis_index("sp") * tok_rows + jnp.arange(tok_rows, dtype=jnp.int32)

    k_heads = prepare_heads(
        key_rows.reshape(tok_rows, local_kv, head_dim), key_gain, positions
    ).reshape(tok_rows, local_kv * head_dim)
    kv = jnp.concatenate([k_heads, value_rows], axis=1)
    far = sp_size // 2
    kv_all = [kv] + travel(kv, onward, far) + travel(kv, backward, sp_size - 1 - far)

    down_half = down_weight.shape[0] // 2
    gate_ring = [gate_weight] + travel(gate_weight, onward, sp_size - 1)
    up_ring = [up_weight] + travel(up_weight, backward, sp_size - 1)
    first_ring = [down_weight[:down_half]]
    first_ring += travel(first_ring[0], onward, sp_size - 1)
    second_ring = [down_weight[down_half:]]
    second_ring += travel(second_ring[0], backward, sp_size - 1)

    q_heads = prepare_heads(query_rows.reshape(tok_rows, local_q, head_dim), query_gain, positions)
    q_stack = (
        q_heads.reshape(tok_rows, local_kv, group_size, head_dim)
        .transpose(1, 2, 0, 3)
        .reshape(local_kv, group_size * tok_rows, head_dim)
    )
    kv_whole = jnp.concatenate(kv_all, axis=0)
    kv_heads = kv_whole.reshape(sp_size * tok_rows, 2, local_kv, head_dim).transpose(1, 2, 0, 3)
    attended = attend(q_stack, kv_heads[0], kv_heads[1])
    attended = (
        attended.reshape(local_kv, group_size, tok_rows, head_dim)
        .transpose(2, 0, 1, 3)
        .reshape(tok_rows, local_q * head_dim)
    )
    own_count = tok_rows // tp_size
    tp_index = lax.axis_index("tp")
    by_peer = [
        lax.dynamic_slice_in_dim(attended, (tp_index ^ d) * own_count, own_count, 0)
        for d in range(tp_size)
    ]

    def summed(parts):
        total = parts[0].astype(jnp.float32)
        arrived = [partner(parts[d], d) for d in range(1, tp_size)]
        for piece in arrived:
            total = total + piece.astype(jnp.float32)
        return total

    head_part = jnp.dot(
        jnp.concatenate(by_peer, axis=0), out_weight, preferred_element_type=jnp.float32
    ).astype(jnp.bfloat16)
    attn_sum = summed([head_part[d * own_count : (d + 1) * own_count] for d in range(tp_size)])
    own_rows = (residual.astype(jnp.float32) + attn_sum).astype(jnp.bfloat16)
    blocks = [row_norm(own_rows, mix_gain)]
    bit = tp_size // 2
    gathered = {0: blocks[0]}
    while bit >= 1:
        for d in list(gathered):
            gathered[d | bit] = partner(gathered[d], bit)
        bit //= 2
    normed_all = jnp.concatenate([gathered[d] for d in range(tp_size)], axis=0)

    depth = gate_weight.shape[0]

    def contracted(pieces, sign):
        total = None
        for k, piece in enumerate(pieces):
            columns = lax.dynamic_slice_in_dim(normed_all, owner(sign * k) * depth, depth, 1)
            term = jnp.dot(columns, piece, preferred_element_type=jnp.float32)
            total = term if total is None else total + term
        return total

    gate_act = contracted(gate_ring, -1)
    up_act = contracted(up_ring, 1)
    hidden = (jax.nn.silu(gate_act) * up_act).astype(jnp.bfloat16)
    width = down_weight.shape[1]
    unit_part = jnp.zeros((tok_rows, width * sp_size), jnp.bfloat16)
    for k in range(sp_size):
        whole = jnp.concatenate([first_ring[k], second_ring[(sp_size - k) % sp_size]], axis=0)
        block = jnp.dot(hidden, whole, preferred_element_type=jnp.float32).astype(jnp.bfloat16)
        unit_part = lax.dynamic_update_slice_in_dim(unit_part, block, owner(-k) * width, 1)
    unit_sum = summed([unit_part[d * own_count : (d + 1) * own_count] for d in range(tp_size)])
    return (own_rows.astype(jnp.float32) + 0.5 * unit_sum).astype(jnp.bfloat16)


def solution(mesh):
    placed = (
        P("sp", "tp"),
        P("sp", "tp"),
        P("sp", "tp"),
        P(),
        P(),
        P(("sp", "tp"), None),
        P("tp", None),
        P(),
        P("sp", "tp"),
        P("sp", "tp"),
        P("tp", "sp"),
    )
    return jax.shard_map(
        functools.partial(on_device, mesh.shape["sp"], mesh.shape["tp"]),
        mesh=mesh,
        in_specs=placed,
        out_specs=P(("sp", "tp"), None),
        check_vma=False,
    )
```

```python
import functools
import math

import jax
import jax.numpy as jnp
from jax import lax
from jax.experimental import pallas as pl
from jax.experimental.pallas import tpu as pltpu
from jax.sharding import PartitionSpec as P

GRID = 64

norm_eps = 1e-06
theta_base = 10000.0


def spin(halfway, angles):
    cosine = jnp.cos(angles)[:, None, :]
    sine_val = jnp.sin(angles)[:, None, :]
    quarter = halfway.shape[-1] // 2
    leading = halfway[..., :quarter]
    trailing = halfway[..., quarter:]
    return [leading * cosine - trailing * sine_val, trailing * cosine + leading * sine_val]


def rotate_grid(vectors, positions):
    head_dim = vectors.shape[-1]
    quarter = head_dim // 4
    frequency = jnp.power(
        theta_base, -2.0 * jnp.arange(quarter, dtype=jnp.float32) / (head_dim // 2)
    )
    row_angle = (positions // GRID).astype(jnp.float32)[:, None] * frequency
    col_angle = (positions % GRID).astype(jnp.float32)[:, None] * frequency
    lower_half = vectors[..., : 2 * quarter]
    upper_half = vectors[..., 2 * quarter :]
    return jnp.concatenate(spin(lower_half, row_angle) + spin(upper_half, col_angle), axis=-1)


def prepare_heads(raw_heads, head_gain, positions):
    floated = raw_heads.astype(jnp.float32)
    scaled = floated * lax.rsqrt(jnp.mean(floated * floated, axis=-1, keepdims=True) + norm_eps)
    return rotate_grid(scaled * head_gain, positions).astype(jnp.bfloat16)


def row_norm(row_data, row_gain):
    floated = row_data.astype(jnp.float32)
    scaled = floated * lax.rsqrt(jnp.mean(floated * floated, axis=-1, keepdims=True) + norm_eps)
    return (scaled * row_gain).astype(jnp.bfloat16)


def attend_body(factor, q_ref, k_ref, v_ref, o_ref):
    scores = lax.dot_general(
        q_ref[0], k_ref[0], (((1,), (1,)), ((), ())), preferred_element_type=jnp.float32
    )
    top = jnp.max(scores, axis=-1, keepdims=True)
    weights = jnp.exp2((scores - top) * factor)
    total = jnp.sum(weights, axis=-1, keepdims=True)
    mixed = jnp.dot(weights.astype(jnp.bfloat16), v_ref[0], preferred_element_type=jnp.float32)
    o_ref[0] = (mixed / total).astype(o_ref.dtype)


def attend(q_stack, keys, values):
    local_kv, rows, head_dim = q_stack.shape
    count = keys.shape[1]
    tile = min(256, rows)
    return pl.pallas_call(
        functools.partial(attend_body, head_dim**-0.5 * math.log2(math.e)),
        grid=(local_kv, rows // tile),
        in_specs=[
            pl.BlockSpec((1, tile, head_dim), lambda h, i: (h, i, 0)),
            pl.BlockSpec((1, count, head_dim), lambda h, i: (h, 0, 0)),
            pl.BlockSpec((1, count, head_dim), lambda h, i: (h, 0, 0)),
        ],
        out_specs=pl.BlockSpec((1, tile, head_dim), lambda h, i: (h, i, 0)),
        out_shape=jax.ShapeDtypeStruct((local_kv, rows, head_dim), jnp.bfloat16),
        compiler_params=pltpu.CompilerParams(vmem_limit_bytes=40 * 1024 * 1024),
        cost_estimate=pl.CostEstimate(
            flops=4 * local_kv * rows * count * head_dim,
            bytes_accessed=4 * local_kv * (rows + count) * head_dim,
            transcendentals=local_kv * rows * count,
        ),
    )(q_stack, keys, values)


def on_device(
    sp_size,
    tp_size,
    query_rows,
    key_rows,
    value_rows,
    query_gain,
    key_gain,
    residual,
    out_weight,
    mix_gain,
    gate_weight,
    up_weight,
    down_weight,
):
    ring = list(range(0, sp_size, 2)) + list(range(1, sp_size, 2))[::-1]
    onward = [(ring[i], ring[(i + 1) % sp_size]) for i in range(sp_size)]
    backward = [(b, a) for a, b in onward]
    sp_index, tp_index = lax.axis_index("sp"), lax.axis_index("tp")

    def travel(piece, perm, steps):
        out = []
        for _ in range(steps):
            piece = lax.ppermute(piece, "sp", perm)
            out.append(piece)
        return out

    def relabel(piece, rule):
        perm = []
        for s in range(sp_size):
            for t in range(tp_size):
                new_s, new_t = rule(s, t)
                perm.append((s * tp_size + t, new_s * tp_size + new_t))
        return lax.ppermute(piece, ("sp", "tp"), perm)

    def flip(piece, sp_mask, tp_mask):
        return relabel(piece, lambda s, t: (s ^ sp_mask, t ^ tp_mask))

    def swap_bits(s, t):
        return (s & ~2) | ((t & 1) << 1), (t & ~1) | ((s >> 1) & 1)

    tok_rows = query_rows.shape[0]
    head_dim = query_gain.shape[0]
    local_kv = key_rows.shape[1] // head_dim
    local_q = query_rows.shape[1] // head_dim
    group_size = local_q // local_kv
    positions = lax.axis_index("sp") * tok_rows + jnp.arange(tok_rows, dtype=jnp.int32)

    k_heads = prepare_heads(
        key_rows.reshape(tok_rows, local_kv, head_dim), key_gain, positions
    ).reshape(tok_rows, local_kv * head_dim)
    kv = jnp.concatenate([k_heads, value_rows], axis=1)
    far = sp_size // 2
    kv_all = [kv] + travel(kv, onward, far) + travel(kv, backward, sp_size - 1 - far)

    bits = [1 << i for i in range(sp_size.bit_length() - 1)]
    order = bits[2:][::-1] + [1, 2]

    def collect(shard, gate_on):
        shard = relabel(shard, swap_bits)
        if gate_on is not None:
            shard, _ = lax.optimization_barrier((shard, gate_on))
        pieces = {0: shard}
        for bit in order:
            for mask in list(pieces):
                if bit == 2:
                    pieces[mask | bit] = flip(pieces[mask], 0, 1)
                else:
                    pieces[mask | bit] = flip(pieces[mask], bit, 0)
        return [pieces[mask] for mask in range(sp_size)]

    gate_on = kv_all[2][:8]
    gate_whole = jnp.concatenate(collect(gate_weight, gate_on), axis=0)
    up_whole = jnp.concatenate(collect(up_weight, gate_on), axis=0)
    down_whole = jnp.concatenate(collect(down_weight, gate_on), axis=1)

    q_heads = prepare_heads(query_rows.reshape(tok_rows, local_q, head_dim), query_gain, positions)
    q_stack = (
        q_heads.reshape(tok_rows, local_kv, group_size, head_dim)
        .transpose(1, 2, 0, 3)
        .reshape(local_kv, group_size * tok_rows, head_dim)
    )
    kv_whole = jnp.concatenate(kv_all, axis=0)
    kv_heads = kv_whole.reshape(sp_size * tok_rows, 2, local_kv, head_dim).transpose(1, 2, 0, 3)
    attended = attend(q_stack, kv_heads[0], kv_heads[1])
    attended = (
        attended.reshape(local_kv, group_size, tok_rows, head_dim)
        .transpose(2, 0, 1, 3)
        .reshape(tok_rows, local_q * head_dim)
    )
    own_count = tok_rows // tp_size
    by_peer = [
        lax.dynamic_slice_in_dim(attended, (tp_index ^ d) * own_count, own_count, 0)
        for d in range(tp_size)
    ]

    def summed(parts, masks):
        total = parts[0].astype(jnp.float32)
        arrived = [flip(piece, *mask) for piece, mask in zip(parts[1:], masks)]
        for piece in arrived:
            total = total + piece.astype(jnp.float32)
        return total

    def row_blocks(array):
        return [array[d * own_count : (d + 1) * own_count] for d in range(tp_size)]

    base = (sp_index & ~2) | ((tp_index & 1) << 1)
    width = down_weight.shape[1]

    def reorder(array):
        return jnp.concatenate(
            [
                lax.dynamic_slice_in_dim(array, (base ^ mask) * width, width, 1)
                for mask in range(sp_size)
            ],
            axis=1,
        )

    head_part = jnp.dot(
        jnp.concatenate(by_peer, axis=0), out_weight, preferred_element_type=jnp.float32
    ).astype(jnp.bfloat16)
    attn_sum = summed(row_blocks(head_part), [(0, d) for d in range(1, tp_size)])
    own_rows = (residual.astype(jnp.float32) + attn_sum).astype(jnp.bfloat16)
    group = [(0, 2), (2, 0), (2, 2)]
    normed = reorder(row_norm(own_rows, mix_gain))
    normed_all = jnp.concatenate([normed] + [flip(normed, *mask) for mask in group], axis=0)
    gate_act = jnp.dot(normed_all, gate_whole, preferred_element_type=jnp.float32)
    up_act = jnp.dot(normed_all, up_whole, preferred_element_type=jnp.float32)
    hidden = (jax.nn.silu(gate_act) * up_act).astype(jnp.bfloat16)
    unit_part = jnp.dot(hidden, down_whole, preferred_element_type=jnp.float32).astype(
        jnp.bfloat16
    )
    unit_sum = reorder(summed(row_blocks(unit_part), group))
    return (own_rows.astype(jnp.float32) + 0.5 * unit_sum).astype(jnp.bfloat16)


def solution(mesh):
    placed = (
        P("sp", "tp"),
        P("sp", "tp"),
        P("sp", "tp"),
        P(),
        P(),
        P(("sp", "tp"), None),
        P("tp", None),
        P(),
        P("sp", "tp"),
        P("sp", "tp"),
        P("tp", "sp"),
    )
    return jax.shard_map(
        functools.partial(on_device, mesh.shape["sp"], mesh.shape["tp"]),
        mesh=mesh,
        in_specs=placed,
        out_specs=P(("sp", "tp"), None),
        check_vma=False,
    )
```

```python
import functools
import math

import jax
import jax.numpy as jnp
from jax import lax
from jax.experimental import pallas as pl
from jax.experimental.pallas import tpu as pltpu
from jax.sharding import PartitionSpec as P

GRID = 64

norm_eps = 1e-06
theta_base = 10000.0


def spin(halfway, angles):
    cosine = jnp.cos(angles)[:, None, :]
    sine_val = jnp.sin(angles)[:, None, :]
    quarter = halfway.shape[-1] // 2
    leading = halfway[..., :quarter]
    trailing = halfway[..., quarter:]
    return [leading * cosine - trailing * sine_val, trailing * cosine + leading * sine_val]


def rotate_grid(vectors, positions):
    head_dim = vectors.shape[-1]
    quarter = head_dim // 4
    frequency = jnp.power(
        theta_base, -2.0 * jnp.arange(quarter, dtype=jnp.float32) / (head_dim // 2)
    )
    row_angle = (positions // GRID).astype(jnp.float32)[:, None] * frequency
    col_angle = (positions % GRID).astype(jnp.float32)[:, None] * frequency
    lower_half = vectors[..., : 2 * quarter]
    upper_half = vectors[..., 2 * quarter :]
    return jnp.concatenate(spin(lower_half, row_angle) + spin(upper_half, col_angle), axis=-1)


def prepare_heads(raw_heads, head_gain, positions):
    floated = raw_heads.astype(jnp.float32)
    scaled = floated * lax.rsqrt(jnp.mean(floated * floated, axis=-1, keepdims=True) + norm_eps)
    return rotate_grid(scaled * head_gain, positions).astype(jnp.bfloat16)


def row_norm(row_data, row_gain):
    floated = row_data.astype(jnp.float32)
    scaled = floated * lax.rsqrt(jnp.mean(floated * floated, axis=-1, keepdims=True) + norm_eps)
    return (scaled * row_gain).astype(jnp.bfloat16)


def attend_body(factor, q_ref, k_ref, v_ref, o_ref):
    scores = lax.dot_general(
        q_ref[0], k_ref[0], (((1,), (1,)), ((), ())), preferred_element_type=jnp.float32
    )
    top = jnp.max(scores, axis=-1, keepdims=True)
    weights = jnp.exp2((scores - top) * factor)
    total = jnp.sum(weights, axis=-1, keepdims=True)
    mixed = jnp.dot(weights.astype(jnp.bfloat16), v_ref[0], preferred_element_type=jnp.float32)
    o_ref[0] = (mixed / total).astype(o_ref.dtype)


def attend(q_stack, keys, values):
    local_kv, rows, head_dim = q_stack.shape
    count = keys.shape[1]
    tile = min(256, rows)
    return pl.pallas_call(
        functools.partial(attend_body, head_dim**-0.5 * math.log2(math.e)),
        grid=(local_kv, rows // tile),
        in_specs=[
            pl.BlockSpec((1, tile, head_dim), lambda h, i: (h, i, 0)),
            pl.BlockSpec((1, count, head_dim), lambda h, i: (h, 0, 0)),
            pl.BlockSpec((1, count, head_dim), lambda h, i: (h, 0, 0)),
        ],
        out_specs=pl.BlockSpec((1, tile, head_dim), lambda h, i: (h, i, 0)),
        out_shape=jax.ShapeDtypeStruct((local_kv, rows, head_dim), jnp.bfloat16),
        compiler_params=pltpu.CompilerParams(vmem_limit_bytes=40 * 1024 * 1024),
        cost_estimate=pl.CostEstimate(
            flops=4 * local_kv * rows * count * head_dim,
            bytes_accessed=4 * local_kv * (rows + count) * head_dim,
            transcendentals=local_kv * rows * count,
        ),
    )(q_stack, keys, values)


def on_device(
    sp_size,
    tp_size,
    query_rows,
    key_rows,
    value_rows,
    query_gain,
    key_gain,
    residual,
    out_weight,
    mix_gain,
    gate_weight,
    up_weight,
    down_weight,
):
    ring = list(range(0, sp_size, 2)) + list(range(1, sp_size, 2))[::-1]
    onward = [(ring[i], ring[(i + 1) % sp_size]) for i in range(sp_size)]
    backward = [(b, a) for a, b in onward]
    sp_index, tp_index = lax.axis_index("sp"), lax.axis_index("tp")

    def travel(piece, perm, steps):
        out = []
        for _ in range(steps):
            piece = lax.ppermute(piece, "sp", perm)
            out.append(piece)
        return out

    def relabel(piece, rule):
        perm = []
        for s in range(sp_size):
            for t in range(tp_size):
                new_s, new_t = rule(s, t)
                if (new_s, new_t) == (s, t):
                    continue
                perm.append((s * tp_size + t, new_s * tp_size + new_t))
        return lax.ppermute(piece, ("sp", "tp"), perm)

    def flip(piece, sp_mask, tp_mask):
        return relabel(piece, lambda s, t: (s ^ sp_mask, t ^ tp_mask))

    def swap_bits(s, t):
        return (s & ~2) | ((t & 1) << 1), (t & ~1) | ((s >> 1) & 1)

    tok_rows = query_rows.shape[0]
    head_dim = query_gain.shape[0]
    local_kv = key_rows.shape[1] // head_dim
    local_q = query_rows.shape[1] // head_dim
    group_size = local_q // local_kv
    positions = lax.axis_index("sp") * tok_rows + jnp.arange(tok_rows, dtype=jnp.int32)

    k_heads = prepare_heads(
        key_rows.reshape(tok_rows, local_kv, head_dim), key_gain, positions
    ).reshape(tok_rows, local_kv * head_dim)
    kv = jnp.concatenate([k_heads, value_rows], axis=1)
    far = sp_size // 2
    kv_all = [kv] + travel(kv, onward, far) + travel(kv, backward, sp_size - 1 - far)

    bits = [1 << i for i in range(sp_size.bit_length() - 1)]
    order = bits[2:][::-1] + [1, 2]

    def collect(shard, gate_on):
        swapped = relabel(shard, swap_bits)
        keeps = ((sp_index >> 1) & 1) == (tp_index & 1)
        shard = jnp.where(keeps, shard, swapped)
        if gate_on is not None:
            shard, _ = lax.optimization_barrier((shard, gate_on))
        pieces = {0: shard}
        for bit in order:
            for mask in list(pieces):
                if bit == 2:
                    pieces[mask | bit] = flip(pieces[mask], 0, 1)
                else:
                    pieces[mask | bit] = flip(pieces[mask], bit, 0)
        return [pieces[mask] for mask in range(sp_size)]

    gate_on = (kv_all[far][:8], kv_all[-1][:8])
    gate_whole = jnp.concatenate(collect(gate_weight, gate_on), axis=0)
    up_whole = jnp.concatenate(collect(up_weight, gate_on), axis=0)
    down_whole = jnp.concatenate(collect(down_weight, gate_on), axis=1)

    q_heads = prepare_heads(query_rows.reshape(tok_rows, local_q, head_dim), query_gain, positions)
    q_stack = (
        q_heads.reshape(tok_rows, local_kv, group_size, head_dim)
        .transpose(1, 2, 0, 3)
        .reshape(local_kv, group_size * tok_rows, head_dim)
    )
    kv_whole = jnp.concatenate(kv_all, axis=0)
    kv_heads = kv_whole.reshape(sp_size * tok_rows, 2, local_kv, head_dim).transpose(1, 2, 0, 3)
    attended = attend(q_stack, kv_heads[0], kv_heads[1])
    attended = (
        attended.reshape(local_kv, group_size, tok_rows, head_dim)
        .transpose(2, 0, 1, 3)
        .reshape(tok_rows, local_q * head_dim)
    )
    own_count = tok_rows // tp_size
    by_peer = [
        lax.dynamic_slice_in_dim(attended, (tp_index ^ d) * own_count, own_count, 0)
        for d in range(tp_size)
    ]

    def summed(parts, masks):
        total = parts[0].astype(jnp.float32)
        arrived = [flip(piece, *mask) for piece, mask in zip(parts[1:], masks)]
        for piece in arrived:
            total = total + piece.astype(jnp.float32)
        return total

    def row_blocks(array):
        return [array[d * own_count : (d + 1) * own_count] for d in range(tp_size)]

    base = (sp_index & ~2) | ((tp_index & 1) << 1)
    width = down_weight.shape[1]

    def reorder(array):
        return jnp.concatenate(
            [
                lax.dynamic_slice_in_dim(array, (base ^ mask) * width, width, 1)
                for mask in range(sp_size)
            ],
            axis=1,
        )

    head_part = jnp.dot(
        jnp.concatenate(by_peer, axis=0), out_weight, preferred_element_type=jnp.float32
    ).astype(jnp.bfloat16)
    attn_sum = summed(row_blocks(head_part), [(0, d) for d in range(1, tp_size)])
    own_rows = (residual.astype(jnp.float32) + attn_sum).astype(jnp.bfloat16)
    group = [(0, 2), (2, 0), (2, 2)]
    normed = reorder(row_norm(own_rows, mix_gain))
    normed_all = jnp.concatenate([normed] + [flip(normed, *mask) for mask in group], axis=0)
    gate_act = jnp.dot(normed_all, gate_whole, preferred_element_type=jnp.float32)
    up_act = jnp.dot(normed_all, up_whole, preferred_element_type=jnp.float32)
    hidden = lax.optimization_barrier((jax.nn.silu(gate_act) * up_act).astype(jnp.bfloat16))
    unit_part = jnp.dot(hidden, down_whole, preferred_element_type=jnp.float32).astype(
        jnp.bfloat16
    )
    unit_sum = reorder(summed(row_blocks(unit_part), group))
    return (own_rows.astype(jnp.float32) + 0.5 * unit_sum).astype(jnp.bfloat16)


def solution(mesh):
    placed = (
        P("sp", "tp"),
        P("sp", "tp"),
        P("sp", "tp"),
        P(),
        P(),
        P(("sp", "tp"), None),
        P("tp", None),
        P(),
        P("sp", "tp"),
        P("sp", "tp"),
        P("tp", "sp"),
    )
    return jax.shard_map(
        functools.partial(on_device, mesh.shape["sp"], mesh.shape["tp"]),
        mesh=mesh,
        in_specs=placed,
        out_specs=P(("sp", "tp"), None),
        check_vma=False,
    )
```

```python
import functools
import math

import jax
import jax.numpy as jnp
from jax import lax
from jax.experimental import pallas as pl
from jax.experimental.pallas import tpu as pltpu
from jax.sharding import PartitionSpec as P

GRID = 64

norm_eps = 1e-06
theta_base = 10000.0


def spin(halfway, angles):
    cosine = jnp.cos(angles)[:, None, :]
    sine_val = jnp.sin(angles)[:, None, :]
    quarter = halfway.shape[-1] // 2
    leading = halfway[..., :quarter]
    trailing = halfway[..., quarter:]
    return [leading * cosine - trailing * sine_val, trailing * cosine + leading * sine_val]


def rotate_grid(vectors, positions):
    head_dim = vectors.shape[-1]
    quarter = head_dim // 4
    frequency = jnp.power(
        theta_base, -2.0 * jnp.arange(quarter, dtype=jnp.float32) / (head_dim // 2)
    )
    row_angle = (positions // GRID).astype(jnp.float32)[:, None] * frequency
    col_angle = (positions % GRID).astype(jnp.float32)[:, None] * frequency
    lower_half = vectors[..., : 2 * quarter]
    upper_half = vectors[..., 2 * quarter :]
    return jnp.concatenate(spin(lower_half, row_angle) + spin(upper_half, col_angle), axis=-1)


def prepare_heads(raw_heads, head_gain, positions):
    floated = raw_heads.astype(jnp.float32)
    scaled = floated * lax.rsqrt(jnp.mean(floated * floated, axis=-1, keepdims=True) + norm_eps)
    return rotate_grid(scaled * head_gain, positions).astype(jnp.bfloat16)


def row_norm(row_data, row_gain):
    floated = row_data.astype(jnp.float32)
    scaled = floated * lax.rsqrt(jnp.mean(floated * floated, axis=-1, keepdims=True) + norm_eps)
    return (scaled * row_gain).astype(jnp.bfloat16)


def attend_body(factor, q_ref, k_ref, v_ref, o_ref):
    scores = lax.dot_general(
        q_ref[0], k_ref[0], (((1,), (1,)), ((), ())), preferred_element_type=jnp.float32
    )
    top = jnp.max(scores, axis=-1, keepdims=True)
    weights = jnp.exp2((scores - top) * factor)
    total = jnp.sum(weights, axis=-1, keepdims=True)
    mixed = jnp.dot(weights.astype(jnp.bfloat16), v_ref[0], preferred_element_type=jnp.float32)
    o_ref[0] = (mixed / total).astype(o_ref.dtype)


def attend(q_stack, keys, values):
    local_kv, rows, head_dim = q_stack.shape
    count = keys.shape[1]
    tile = min(256, rows)
    return pl.pallas_call(
        functools.partial(attend_body, head_dim**-0.5 * math.log2(math.e)),
        grid=(local_kv, rows // tile),
        in_specs=[
            pl.BlockSpec((1, tile, head_dim), lambda h, i: (h, i, 0)),
            pl.BlockSpec((1, count, head_dim), lambda h, i: (h, 0, 0)),
            pl.BlockSpec((1, count, head_dim), lambda h, i: (h, 0, 0)),
        ],
        out_specs=pl.BlockSpec((1, tile, head_dim), lambda h, i: (h, i, 0)),
        out_shape=jax.ShapeDtypeStruct((local_kv, rows, head_dim), jnp.bfloat16),
        compiler_params=pltpu.CompilerParams(vmem_limit_bytes=40 * 1024 * 1024),
        cost_estimate=pl.CostEstimate(
            flops=4 * local_kv * rows * count * head_dim,
            bytes_accessed=4 * local_kv * (rows + count) * head_dim,
            transcendentals=local_kv * rows * count,
        ),
    )(q_stack, keys, values)


def on_device(
    sp_size,
    tp_size,
    query_rows,
    key_rows,
    value_rows,
    query_gain,
    key_gain,
    residual,
    out_weight,
    mix_gain,
    gate_weight,
    up_weight,
    down_weight,
):
    ring = list(range(0, sp_size, 2)) + list(range(1, sp_size, 2))[::-1]
    onward = [(ring[i], ring[(i + 1) % sp_size]) for i in range(sp_size)]
    backward = [(b, a) for a, b in onward]
    sp_index, tp_index = lax.axis_index("sp"), lax.axis_index("tp")

    def travel(piece, perm, steps):
        out = []
        for _ in range(steps):
            piece = lax.ppermute(piece, "sp", perm)
            out.append(piece)
        return out

    def relabel(piece, rule):
        perm = []
        for s in range(sp_size):
            for t in range(tp_size):
                new_s, new_t = rule(s, t)
                if (new_s, new_t) == (s, t):
                    continue
                perm.append((s * tp_size + t, new_s * tp_size + new_t))
        return lax.ppermute(piece, ("sp", "tp"), perm)

    def flip(piece, sp_mask, tp_mask):
        return relabel(piece, lambda s, t: (s ^ sp_mask, t ^ tp_mask))

    def swap_bits(s, t):
        return (s & ~2) | ((t & 1) << 1), (t & ~1) | ((s >> 1) & 1)

    tok_rows = query_rows.shape[0]
    head_dim = query_gain.shape[0]
    local_kv = key_rows.shape[1] // head_dim
    local_q = query_rows.shape[1] // head_dim
    group_size = local_q // local_kv
    positions = lax.axis_index("sp") * tok_rows + jnp.arange(tok_rows, dtype=jnp.int32)

    k_heads = prepare_heads(
        key_rows.reshape(tok_rows, local_kv, head_dim), key_gain, positions
    ).reshape(tok_rows, local_kv * head_dim)
    kv = jnp.concatenate([k_heads, value_rows], axis=1)
    far = sp_size // 2
    kv_all = [kv] + travel(kv, onward, far) + travel(kv, backward, sp_size - 1 - far)

    bits = [1 << i for i in range(sp_size.bit_length() - 1)]
    order = bits[2:][::-1] + [1, 2]

    def exchange(shard):
        swapped = relabel(shard, swap_bits)
        keeps = ((sp_index >> 1) & 1) == (tp_index & 1)
        return jnp.where(keeps, shard, swapped)

    def collect(shard, gate_on, early):
        pieces = {0: shard}
        for bit in early:
            for mask in list(pieces):
                pieces[mask | bit] = flip(pieces[mask], bit, 0)
        pieces = {mask: exchange(piece) for mask, piece in pieces.items()}
        for mask in list(pieces):
            pieces[mask], _ = lax.optimization_barrier((pieces[mask], gate_on))
        for bit in order[len(early) :]:
            for mask in list(pieces):
                if bit == 2:
                    pieces[mask | bit] = flip(pieces[mask], 0, 1)
                else:
                    pieces[mask | bit] = flip(pieces[mask], bit, 0)
        return [pieces[mask] for mask in range(sp_size)]

    gate_on = kv_all[max(far - 1, 1)][:8]
    gate_whole = jnp.concatenate(collect(gate_weight, gate_on, order[:1]), axis=0)
    up_whole = jnp.concatenate(collect(up_weight, gate_on, []), axis=0)
    down_whole = jnp.concatenate(collect(down_weight, gate_on, []), axis=1)

    q_heads = prepare_heads(query_rows.reshape(tok_rows, local_q, head_dim), query_gain, positions)
    q_stack = (
        q_heads.reshape(tok_rows, local_kv, group_size, head_dim)
        .transpose(1, 2, 0, 3)
        .reshape(local_kv, group_size * tok_rows, head_dim)
    )
    kv_whole = jnp.concatenate(kv_all, axis=0)
    kv_heads = kv_whole.reshape(sp_size * tok_rows, 2, local_kv, head_dim).transpose(1, 2, 0, 3)
    attended = attend(q_stack, kv_heads[0], kv_heads[1])
    attended = (
        attended.reshape(local_kv, group_size, tok_rows, head_dim)
        .transpose(2, 0, 1, 3)
        .reshape(tok_rows, local_q * head_dim)
    )
    own_count = tok_rows // tp_size
    by_peer = [
        lax.dynamic_slice_in_dim(attended, (tp_index ^ d) * own_count, own_count, 0)
        for d in range(tp_size)
    ]

    def summed(parts, masks):
        total = parts[0].astype(jnp.float32)
        arrived = [flip(piece, *mask) for piece, mask in zip(parts[1:], masks)]
        for piece in arrived:
            total = total + piece.astype(jnp.float32)
        return total

    def row_blocks(array):
        return [array[d * own_count : (d + 1) * own_count] for d in range(tp_size)]

    base = (sp_index & ~2) | ((tp_index & 1) << 1)
    width = down_weight.shape[1]

    def reorder(array):
        return jnp.concatenate(
            [
                lax.dynamic_slice_in_dim(array, (base ^ mask) * width, width, 1)
                for mask in range(sp_size)
            ],
            axis=1,
        )

    head_part = jnp.dot(
        jnp.concatenate(by_peer, axis=0), out_weight, preferred_element_type=jnp.float32
    ).astype(jnp.bfloat16)
    attn_sum = summed(row_blocks(head_part), [(0, d) for d in range(1, tp_size)])
    own_rows = (residual.astype(jnp.float32) + attn_sum).astype(jnp.bfloat16)
    group = [(0, 2), (2, 0), (2, 2)]
    normed = reorder(row_norm(own_rows, mix_gain))
    normed_all = jnp.concatenate([normed] + [flip(normed, *mask) for mask in group], axis=0)
    gate_act = jnp.dot(normed_all, gate_whole, preferred_element_type=jnp.float32)
    up_act = jnp.dot(normed_all, up_whole, preferred_element_type=jnp.float32)
    hidden = lax.optimization_barrier((jax.nn.silu(gate_act) * up_act).astype(jnp.bfloat16))
    unit_part = jnp.dot(hidden, down_whole, preferred_element_type=jnp.float32).astype(
        jnp.bfloat16
    )
    unit_sum = reorder(summed(row_blocks(unit_part), group))
    return (own_rows.astype(jnp.float32) + 0.5 * unit_sum).astype(jnp.bfloat16)


def solution(mesh):
    placed = (
        P("sp", "tp"),
        P("sp", "tp"),
        P("sp", "tp"),
        P(),
        P(),
        P(("sp", "tp"), None),
        P("tp", None),
        P(),
        P("sp", "tp"),
        P("sp", "tp"),
        P("tp", "sp"),
    )
    return jax.shard_map(
        functools.partial(on_device, mesh.shape["sp"], mesh.shape["tp"]),
        mesh=mesh,
        in_specs=placed,
        out_specs=P(("sp", "tp"), None),
        check_vma=False,
    )
```
